256 devices in a mesh: grp: 4 (over y, x), ep: 32 (over z), tp: 2 (over core).
Axes of the slice: x: 2, y: 2, z: 32, core: 2. Of those that a mesh axis runs over, the one named last changes fastest.
The devices are a block of a 4x8x32 slice.
Arguments:
- tokens: bfloat16 [65536, 2048], P(('grp', 'ep', 'tp')), parts along dimension 0, may hold values from -6 to 6
- norm_gain: float32 [2048], replicated, may hold values from 0.1 to 1.9
- expert_ids: int32 [65536, 2], P(('grp', 'ep', 'tp')), parts along dimension 0, may hold values from 0 to 31, all different within a row; in each aligned block of 256 rows (0 to 255, 256 to 511, ...) at most 24 rows name the same one
- route_weights: float32 [65536, 2], P(('grp', 'ep', 'tp')), parts along dimension 0, may hold values from 0.05 to 1
- w_gate: bfloat16 [32, 2048, 1024], P('ep', None, 'tp'), may hold values from -0.125 to 0.125
- w_up: bfloat16 [32, 2048, 1024], P('ep', None, 'tp'), may hold values from -0.125 to 0.125
- w_down: bfloat16 [32, 1024, 2048], P('ep', 'tp'), may hold values from -0.1875 to 0.1875
Outputs:
- mixed: bfloat16 [65536, 2048], P(('grp', 'ep', 'tp')), parts along dimension 0
The draws below stay inside these ranges and needn't reach their ends.
There are 4 independent parts, one for each index of `grp`. The reference program is written for one: setup_inputs(seed, part) draws one part's arguments, and reference() takes and returns one part's arrays. A program takes and returns all parts, laid end to end along the dimension named above; an argument that names none is the same for every part. Nothing has to cross between parts.
Inputs may be any that keep to these rules, and one draw needn't show every extreme that they name: `expert_ids`: each row names 2 different experts. Among the rows of one device no expert is named more than 24 times, and in every draw some expert is named exactly 24 times by the rows of some device.
All inputs are finite; a program needn't handle non-finite values.
Results may differ from the reference program's by a relative error of at most 0.0071.
Values may be sent and summed in bfloat16 or wider, within the bound.
No kernel may reach another device: no remote copies, remote signals or barrier semaphores. Data moves between devices by JAX's collectives and lax.ppermute only.
A program may use at most 128 MiB of HBM per device.

```python
import math
import jax
import jax.numpy as jnp
import numpy as np
from jax import lax

D = 2048
DE = 1024
TOP_K = 2
TOK_DEV = 256
EXPERTS = 32
TOKENS = 16384
CAP = 24


def block_scale(own_key, shape, pieces, low, top_value):
    def one(axis_at, blocks):
        heights = jax.random.uniform(jax.random.fold_in(jax.random.fold_in(own_key, 6), axis_at), (blocks,), jnp.float32, low / len(pieces), top_value / len(pieces))
        return jnp.repeat(jnp.exp(heights), shape[axis_at] // blocks).reshape((-1,) + (1,) * (len(shape) - axis_at - 1))

    factor_of = one(*pieces[0])
    for cut in pieces[1:]:
        factor_of = factor_of * one(*cut)
    return factor_of


def assign_block(own_key, own, number, rows, amount, top, most, skew):
    ranking = jax.random.permutation(own_key, amount)
    crowded, usual = shares(amount, rows * top, most, skew, True), shares(amount, rows * top, most, skew, False)
    places = jnp.arange(amount)

    def named(lengths, rotation):
        used = int((lengths > 0).sum())
        fixed = max(1, used // 4)
        moved = fixed + (places - fixed + rotation * (used - fixed)) % max(1, amount - fixed)
        return jnp.zeros((amount,), jnp.int32).at[ranking[jnp.where(places < fixed, places, moved)]].set(jnp.asarray(lengths, jnp.int32))

    lengths = jnp.where(number % 4 == 0, named(crowded, number // 4), named(usual, number - number // 4 - 1))
    mixed = jax.random.permutation(jax.random.fold_in(own, 3), amount)
    donor, taker = mixed[0:amount // 2 * 2:2], mixed[1:amount // 2 * 2:2]
    margin = jnp.minimum(lengths[donor] - 1, most - lengths[taker]) // 2
    margin = jnp.where((donor == ranking[0]) | (taker == ranking[0]) | (lengths[taker] == 0), 0, jnp.maximum(margin, 0))
    moved = jax.random.randint(jax.random.fold_in(own, 4), (amount // 2,), 0, 1 << 20) % (margin + 1)
    lengths = lengths.at[donor].add(-moved).at[taker].add(moved)
    items = jnp.searchsorted(jnp.cumsum(lengths), jnp.arange(rows * top), side="right").astype(jnp.int32)
    table = items.reshape(top, rows).T
    table = table[jax.random.permutation(jax.random.fold_in(own, 1), rows)]
    rotation = jax.random.randint(jax.random.fold_in(own, 2), (rows, 1), 0, top)
    return jnp.take_along_axis(table, (jnp.arange(top)[None, :] + rotation) % top, axis=1)


def shares(count, total, reach, lean, full):
    portions = [(1 << 20) // math.isqrt(grade ** lean) + 1 for grade in range(1, count + 1)]
    largest = reach if full else min(reach, max(-(-total // count), total * portions[0] // sum(portions)))
    least = 1 if total - largest >= count - 1 else 0
    given, surplus = [largest] + [least] * (count - 1), total - largest - least * (count - 1)
    while surplus > 0:
        candidates = [i for i in range(1, count) if given[i] < largest] or [i for i in range(1, count) if given[i] < reach]
        whole, budget = sum([portions[i] for i in candidates]), surplus
        for i in candidates:
            addition = min(reach - given[i], max(1, budget * portions[i] // whole), surplus)
            given[i] = given[i] + addition
            surplus = surplus - addition
    return np.array(given)


def centred(stream_key, shape, deviation, reach, shards=(), kind=jnp.bfloat16):
    entries = jax.random.normal(stream_key, shape, jnp.float32) * deviation
    if len(shards) > 0:
        entries = block_scale(stream_key, shape, shards, -0.22, 0.18) * entries
    return jnp.clip(entries, min=-reach, max=reach).astype(kind)


def setup_inputs(seed: int = 0, part: int = 0) -> dict:
    arg_keys = jax.random.split(jax.random.key(seed), 8)
    part_splits = jax.random.split(jax.random.fold_in(arg_keys[7], part), 8)
    tokens = centred(part_splits[0], (TOKENS, D), 1.0, 6.0, ((0, 64),))
    norm_gain = jnp.clip(1.0 + 0.18 * jax.random.normal(arg_keys[1], (D,), jnp.float32), 0.1, 1.9)
    expert_ids_keys = jax.random.split(jax.random.fold_in(part_splits[2], 1), TOKENS // TOK_DEV)
    expert_ids_turns = jax.random.permutation(jax.random.fold_in(part_splits[2], 3), TOKENS // TOK_DEV)
    expert_ids = jax.vmap(lambda own, number: assign_block(jax.random.fold_in(part_splits[2], 2), own, number, TOK_DEV, EXPERTS, TOP_K, CAP, 2))(expert_ids_keys, expert_ids_turns).reshape((TOKENS, TOP_K))
    route_weights = jnp.clip(jnp.exp(math.log(1.0) - 2.9957323 * jax.random.uniform(part_splits[3], (TOKENS, TOP_K), jnp.float32) ** block_scale(part_splits[3], (TOKENS, TOP_K), ((0, 64),), -0.2, 0.2)), 0.05, 1.0)
    w_gate = centred(arg_keys[4], (EXPERTS, D, DE), D ** -0.5, 0.125, ((0, 32), (2, 2)))
    w_up = centred(arg_keys[5], (EXPERTS, D, DE), D ** -0.5, 0.125, ((0, 32), (2, 2)))
    w_down = centred(arg_keys[6], (EXPERTS, DE, D), DE ** -0.5, 0.1875, ((0, 32), (1, 2)))
    return dict(tokens=tokens, norm_gain=norm_gain, expert_ids=expert_ids, route_weights=route_weights, w_gate=w_gate, w_up=w_up, w_down=w_down)


def reference(tokens, norm_gain, expert_ids, route_weights, w_gate, w_up, w_down):
    values = tokens.astype(jnp.float32)
    scale = lax.rsqrt(lax.optimization_barrier(jnp.mean(values * values, axis=-1, keepdims=True)) + 1e-06)
    normed = (values * scale * norm_gain).astype(jnp.bfloat16)
    flat_ids = expert_ids.reshape(-1)
    flat_weights = route_weights.reshape(-1)
    total_rows = TOKENS // TOK_DEV * CAP

    def per_expert(carry, expert):
        chosen = flat_ids == expert
        count = jnp.sum(chosen.astype(jnp.int32))
        picks = jnp.nonzero(chosen, size=total_rows, fill_value=0)[0].astype(jnp.int32)
        live = jnp.arange(total_rows, dtype=jnp.int32) < count
        token_rows = picks // TOP_K
        rows = normed[token_rows]
        gate = jnp.dot(rows, w_gate[expert], preferred_element_type=jnp.float32)
        upper = jnp.dot(rows, w_up[expert], preferred_element_type=jnp.float32)
        hidden = (jax.nn.silu(gate) * upper).astype(jnp.bfloat16)
        result = jnp.dot(hidden, w_down[expert], preferred_element_type=jnp.float32).astype(jnp.bfloat16)
        result = lax.optimization_barrier(result).astype(jnp.float32)
        weight = jnp.where(live, flat_weights[picks], jnp.float32(0.0))
        carry = carry.at[token_rows].add(weight[:, None] * result)
        return (carry, None)
    start = jnp.zeros((TOKENS, D), jnp.float32)
    total, _ = lax.scan(per_expert, start, jnp.arange(EXPERTS, dtype=jnp.int32))
    return total.astype(jnp.bfloat16)
```

```python
import jax
import jax.numpy as jnp
from jax import lax
from jax.experimental import pallas as pl
from jax.experimental.pallas import tpu as pltpu
from jax.sharding import PartitionSpec as P


F32, BF16, I32 = jnp.float32, jnp.bfloat16, jnp.int32
VMEM = pl.BlockSpec(memory_space=pltpu.VMEM)
SMEM = pl.BlockSpec(memory_space=pltpu.SMEM)
MIB = 1 << 20


def dot(a, b):
    return jnp.dot(a, b, preferred_element_type=F32)


def one_hot(pick):
    return pick.astype(F32).astype(BF16)


def place_kernel(experts, slots, me_ref, ids_ref, tokens_ref, gain_ref, pos_ref, send_ref):
    rows = tokens_ref.shape[0]
    values = tokens_ref[...].astype(F32)
    scale = lax.rsqrt(jnp.mean(values * values, axis=-1, keepdims=True) + 1e-06)
    normed = (values * scale * gain_ref[...]).astype(BF16)
    earlier = one_hot(
        lax.broadcasted_iota(I32, (rows, rows), 0) < lax.broadcasted_iota(I32, (rows, rows), 1)
    )
    names = lax.broadcasted_iota(I32, (experts, rows), 0)
    taken = jnp.zeros((experts, 1), F32)
    places = []
    for k in range(ids_ref.shape[0]):
        ids = ids_ref[k : k + 1, :]
        hot = (names == ids).astype(F32)
        before = dot(hot.astype(BF16), earlier) + taken
        taken = taken + jnp.sum(hot, axis=1, keepdims=True)
        slot = jnp.sum(hot * before, axis=0, keepdims=True).astype(I32)
        away = ids - me_ref[0]
        away = jnp.where(away < 0, away + experts, away)
        near = jnp.where(2 * away <= experts, 2 * away - 1, 2 * (experts - away))
        near = jnp.where(away == 0, 0, near)
        pos = near * slots + slot
        pos_ref[k : k + 1, :] = pos
        places.append(pos)
    chunk = 128
    for start in range(0, experts * slots, chunk):
        at = lax.broadcasted_iota(I32, (chunk, rows), 0) + start
        pick = at == places[0]
        for pos in places[1:]:
            pick = pick | (at == pos)
        send_ref[start : start + chunk, :] = dot(one_hot(pick), normed).astype(BF16)


def weigh(start, pos_ref, weights_ref, parts):
    rows = jnp.concatenate([p[...] for p in parts], axis=0)
    total = None
    for k in range(pos_ref.shape[1]):
        at = lax.broadcasted_iota(I32, (pos_ref.shape[0], rows.shape[0]), 1) + start
        pick = one_hot(at == pos_ref[:, k : k + 1])
        part = weights_ref[:, k : k + 1] * dot(pick, rows)
        total = part if total is None else total + part
    return total


def first_mix_kernel(pos_ref, weights_ref, *refs):
    refs[-1][...] = weigh(0, pos_ref, weights_ref, refs[:-1])


def last_mix_kernel(start, pos_ref, weights_ref, sofar_ref, *refs):
    refs[-1][...] = (sofar_ref[...] + weigh(start, pos_ref, weights_ref, refs[:-1])).astype(BF16)


def call(kernel, out, operands, limit, specs=None):
    return pl.pallas_call(
        kernel,
        out_shape=out,
        in_specs=specs or [VMEM] * len(operands),
        out_specs=jax.tree.map(lambda _: VMEM, out),
        compiler_params=pltpu.CompilerParams(vmem_limit_bytes=limit * MIB),
    )(*operands)


def per_device(tokens, norm_gain, expert_ids, route_weights, w_gate, w_up, w_down):
    tok_rows, width = tokens.shape
    top_count = expert_ids.shape[1]
    ep_size, tp_size = lax.axis_size("ep"), lax.axis_size("tp")
    experts = w_gate.shape[0] * ep_size
    slots = 3 * tok_rows * top_count // (2 * experts)

    def sds(shape, dtype):
        return jax.ShapeDtypeStruct(shape, dtype)

    order = [0]
    for d in range(1, ep_size // 2 + 1):
        order += [d] if 2 * d == ep_size else [d, -d]
    first = 2 * 11 + 1

    me = lax.axis_index("ep").astype(I32)[None]
    pos, send = call(
        lambda *refs: place_kernel(experts, slots, *refs),
        (sds((top_count, tok_rows), I32), sds((experts * slots, width), BF16)),
        (me, expert_ids.T, tokens, norm_gain[None, :]),
        24,
        [SMEM, VMEM, VMEM, VMEM],
    )

    swap = [(i, (i + 1) % tp_size) for i in range(tp_size)]

    def whole(w, axis):
        return jnp.concatenate([w, lax.ppermute(w, "tp", swap)], axis=axis)

    def shift(rows, d):
        if d == 0:
            return rows
        return lax.ppermute(rows, "ep", [(i, (i + d) % ep_size) for i in range(ep_size)])

    gate_full, up_full, down_full = whole(w_gate[0], 1), whole(w_up[0], 1), whole(w_down[0], 0)

    def expert(rows):
        hidden = (jax.nn.silu(dot(rows, gate_full)) * dot(rows, up_full)).astype(BF16)
        return dot(hidden, down_full).astype(BF16)

    arrived = []
    for i, d in enumerate(order):
        arrived.append(shift(send[i * slots : (i + 1) * slots], d))
    back, result = [], None
    for lo, hi in ((0, first), (first, len(order))):
        if result is not None:
            arrived, _ = lax.optimization_barrier((arrived, result))
        result = expert(jnp.concatenate(arrived[lo:hi], axis=0))
        back += [shift(result[i * slots : (i + 1) * slots], -d) for i, d in enumerate(order[lo:hi])]
    cols = pos.T
    sofar = call(
        first_mix_kernel,
        sds((tok_rows, width), F32),
        (cols, route_weights, *back[:first]),
        24,
    )
    return call(
        lambda *refs: last_mix_kernel(first * slots, *refs),
        sds((tok_rows, width), BF16),
        (cols, route_weights, sofar, *back[first:]),
        24,
    )


def solution(mesh):
    in_specs = (
        P(("grp", "ep", "tp"), None),
        P(),
        P(("grp", "ep", "tp"), None),
        P(("grp", "ep", "tp"), None),
        P("ep", None, "tp"),
        P("ep", None, "tp"),
        P("ep", "tp", None),
    )
    out_specs = P(("grp", "ep", "tp"), None)

    return jax.shard_map(
        per_device, mesh=mesh, in_specs=in_specs, out_specs=out_specs, check_vma=False
    )
```

```python
import jax
import jax.numpy as jnp
from jax import lax
from jax.experimental import pallas as pl
from jax.experimental.pallas import tpu as pltpu
from jax.sharding import PartitionSpec as P


F32, BF16, I32 = jnp.float32, jnp.bfloat16, jnp.int32
VMEM = pl.BlockSpec(memory_space=pltpu.VMEM)
SMEM = pl.BlockSpec(memory_space=pltpu.SMEM)
MIB = 1 << 20


def dot(a, b):
    return jnp.dot(a, b, preferred_element_type=F32)


def one_hot(pick):
    return pick.astype(F32).astype(BF16)


def place_kernel(experts, slots, me_ref, ids_ref, tokens_ref, gain_ref, pos_ref, send_ref):
    rows = tokens_ref.shape[0]
    values = tokens_ref[...].astype(F32)
    scale = lax.rsqrt(jnp.mean(values * values, axis=-1, keepdims=True) + 1e-06)
    normed = (values * scale * gain_ref[...]).astype(BF16)
    earlier = one_hot(
        lax.broadcasted_iota(I32, (rows, rows), 0) < lax.broadcasted_iota(I32, (rows, rows), 1)
    )
    names = lax.broadcasted_iota(I32, (experts, rows), 0)
    taken = jnp.zeros((experts, 1), F32)
    places = []
    for k in range(ids_ref.shape[0]):
        ids = ids_ref[k : k + 1, :]
        hot = (names == ids).astype(F32)
        before = dot(hot.astype(BF16), earlier) + taken
        taken = taken + jnp.sum(hot, axis=1, keepdims=True)
        slot = jnp.sum(hot * before, axis=0, keepdims=True).astype(I32)
        away = ids - me_ref[0]
        away = jnp.where(away < 0, away + experts, away)
        near = jnp.where(2 * away <= experts, 2 * away - 1, 2 * (experts - away))
        near = jnp.where(away == 0, 0, near)
        pos = near * slots + slot
        pos_ref[k : k + 1, :] = pos
        places.append(pos)
    chunk = 128
    for start in range(0, experts * slots, chunk):
        at = lax.broadcasted_iota(I32, (chunk, rows), 0) + start
        pick = at == places[0]
        for pos in places[1:]:
            pick = pick | (at == pos)
        send_ref[start : start + chunk, :] = dot(one_hot(pick), normed).astype(BF16)


def weigh(start, pos_ref, weights_ref, parts):
    rows = jnp.concatenate([p[...] for p in parts], axis=0)
    total = None
    for k in range(pos_ref.shape[1]):
        at = lax.broadcasted_iota(I32, (pos_ref.shape[0], rows.shape[0]), 1) + start
        pick = one_hot(at == pos_ref[:, k : k + 1])
        part = weights_ref[:, k : k + 1] * dot(pick, rows)
        total = part if total is None else total + part
    return total


def first_mix_kernel(pos_ref, weights_ref, *refs):
    refs[-1][...] = weigh(0, pos_ref, weights_ref, refs[:-1])


def last_mix_kernel(start, pos_ref, weights_ref, sofar_ref, *refs):
    refs[-1][...] = (sofar_ref[...] + weigh(start, pos_ref, weights_ref, refs[:-1])).astype(BF16)


def settle_kernel(in_ref, out_ref):
    out_ref[...] = jnp.maximum(in_ref[...], 0)


def call(kernel, out, operands, limit, specs=None):
    return pl.pallas_call(
        kernel,
        out_shape=out,
        in_specs=specs or [VMEM] * len(operands),
        out_specs=jax.tree.map(lambda _: VMEM, out),
        compiler_params=pltpu.CompilerParams(vmem_limit_bytes=limit * MIB),
    )(*operands)


def per_device(tokens, norm_gain, expert_ids, route_weights, w_gate, w_up, w_down):
    tok_rows, width = tokens.shape
    top_count = expert_ids.shape[1]
    ep_size, tp_size = lax.axis_size("ep"), lax.axis_size("tp")
    experts = w_gate.shape[0] * ep_size
    slots = 3 * tok_rows * top_count // (2 * experts)

    def sds(shape, dtype):
        return jax.ShapeDtypeStruct(shape, dtype)

    order = [0]
    for d in range(1, ep_size // 2 + 1):
        order += [d] if 2 * d == ep_size else [d, -d]
    first = 2 * 11 + 1

    me = lax.axis_index("ep").astype(I32)[None]
    pos, send = call(
        lambda *refs: place_kernel(experts, slots, *refs),
        (sds((top_count, tok_rows), I32), sds((experts * slots, width), BF16)),
        (me, expert_ids.T, tokens, norm_gain[None, :]),
        24,
        [SMEM, VMEM, VMEM, VMEM],
    )

    swap = [(i, (i + 1) % tp_size) for i in range(tp_size)]

    def whole(w, axis):
        return jnp.concatenate([w, lax.ppermute(w, "tp", swap)], axis=axis)

    def shift(rows, d):
        if d == 0:
            return rows
        return lax.ppermute(rows, "ep", [(i, (i + d) % ep_size) for i in range(ep_size)])

    gate_full, up_full, down_full = whole(w_gate[0], 1), whole(w_up[0], 1), whole(w_down[0], 0)

    def expert(rows):
        hidden = (jax.nn.silu(dot(rows, gate_full)) * dot(rows, up_full)).astype(BF16)
        return dot(hidden, down_full).astype(BF16)

    parts = ((0, first), (first, len(order)))

    def in_turn(lo, hi):
        out = []
        while lo < hi:
            out += [i for i in (hi - 1, hi - 2) if i >= lo]
            hi -= 2
            out += [i for i in (lo, lo + 1) if i < hi]
            lo += 2
        return out

    arrived, back, result = [None] * len(order), [None] * len(order), None
    for lo, hi in parts:
        for i in in_turn(lo, hi):
            arrived[i] = shift(send[i * slots : (i + 1) * slots], order[i])
    for lo, hi in parts:
        if result is not None:
            arrived, _ = lax.optimization_barrier((arrived, result))
        result = expert(jnp.concatenate(arrived[lo:hi], axis=0))
        for i in in_turn(lo, hi):
            back[i] = shift(result[(i - lo) * slots : (i - lo + 1) * slots], -order[i])
    pos = call(settle_kernel, sds(pos.shape, I32), (pos,), 1)
    cols = pos.T
    sofar = call(
        first_mix_kernel,
        sds((tok_rows, width), F32),
        (cols, route_weights, *back[:first]),
        24,
    )
    return call(
        lambda *refs: last_mix_kernel(first * slots, *refs),
        sds((tok_rows, width), BF16),
        (cols, route_weights, sofar, *back[first:]),
        24,
    )


def solution(mesh):
    in_specs = (
        P(("grp", "ep", "tp"), None),
        P(),
        P(("grp", "ep", "tp"), None),
        P(("grp", "ep", "tp"), None),
        P("ep", None, "tp"),
        P("ep", None, "tp"),
        P("ep", "tp", None),
    )
    out_specs = P(("grp", "ep", "tp"), None)

    return jax.shard_map(
        per_device, mesh=mesh, in_specs=in_specs, out_specs=out_specs, check_vma=False
    )
```

```python
import functools

import jax
import jax.numpy as jnp
from jax import lax
from jax.experimental import pallas as pl
from jax.experimental.pallas import tpu as pltpu
from jax.sharding import PartitionSpec as P


F32, BF16, I32 = jnp.float32, jnp.bfloat16, jnp.int32
VMEM = pl.BlockSpec(memory_space=pltpu.VMEM)
SMEM = pl.BlockSpec(memory_space=pltpu.SMEM)
MIB = 1 << 20


def dot(a, b):
    return jnp.dot(a, b, preferred_element_type=F32)


def one_hot(pick):
    return pick.astype(F32).astype(BF16)


def slots_of(ids, experts):
    rows = ids[0].shape[1]
    earlier = one_hot(
        lax.broadcasted_iota(I32, (rows, rows), 0) < lax.broadcasted_iota(I32, (rows, rows), 1)
    )
    names = lax.broadcasted_iota(I32, (experts, rows), 0)
    taken, out = jnp.zeros((experts, 1), F32), []
    for named in ids:
        hot = (names == named).astype(F32)
        before = dot(hot.astype(BF16), earlier) + taken
        taken = taken + jnp.sum(hot, axis=1, keepdims=True)
        out.append(jnp.sum(hot * before, axis=0, keepdims=True).astype(I32))
    return out


def ahead(named, me, sign, experts):
    away = (named - me) * sign
    away = jnp.where(away < 0, away + experts, away)
    return jnp.where(away >= experts, away - experts, away)


def pick_rows(places, start, count, values):
    at = lax.broadcasted_iota(I32, (count, values.shape[0]), 0) + start
    pick = at == places[0]
    for place in places[1:]:
        pick = pick | (at == place)
    return dot(one_hot(pick), values).astype(BF16)


def place_kernel(experts, slots, me_ref, ids_ref, tokens_ref, gain_ref, pos_ref, block_ref, own_ref):
    rows = tokens_ref.shape[0]
    values = tokens_ref[...].astype(F32)
    scale = lax.rsqrt(jnp.mean(values * values, axis=-1, keepdims=True) + 1e-06)
    normed = (values * scale * gain_ref[...]).astype(BF16)
    block_ref[:rows, :] = normed
    tops = ids_ref.shape[0]
    ids = [ids_ref[k : k + 1, :] for k in range(tops)]
    tail = block_ref.shape[0] - rows
    block_ref[rows:, :] = jnp.zeros((tail, block_ref.shape[1]), BF16)
    for k in range(tops):
        block_ref[rows:, k * rows : (k + 1) * rows] = jnp.broadcast_to(
            ids[k].astype(F32), (tail, rows)
        ).astype(BF16)
    places = []
    for k, slot in enumerate(slots_of(ids, experts)):
        away = ahead(ids[k], me_ref[0], 1, experts)
        near = jnp.where(2 * away <= experts, 2 * away - 1, 2 * (experts - away))
        near = jnp.where(away == 0, 0, near)
        pos_ref[k : k + 1, :] = near * slots + slot
        own = jnp.where(away == 0, slot, slots + slot)
        places.append(jnp.where((away == 0) | (2 * away == experts), own, -1))
    own_ref[...] = pick_rows(places, 0, own_ref.shape[0], normed)


def relay_kernel(experts, slots, sign, me_ref, block_ref, out_ref):
    tail = 8
    rows = block_ref.shape[0] - tail
    tops = 2
    named = block_ref[rows:, : tops * rows].astype(F32).astype(I32)[0:1, :]
    ids = [named[:, k * rows : (k + 1) * rows] for k in range(tops)]
    places = []
    for k, slot in enumerate(slots_of(ids, experts)):
        places.append(ahead(ids[k], me_ref[0], sign, experts) * slots + slot)
    values = block_ref[:rows, :]
    chunk = slots * 7 if out_ref.shape[0] > slots else slots
    for start in range(0, out_ref.shape[0], chunk):
        out_ref[start : start + chunk, :] = pick_rows(places, start, chunk, values)


def weigh(start, pos_ref, weights_ref, parts):
    rows = jnp.concatenate([p[...] for p in parts], axis=0)
    total = None
    for k in range(pos_ref.shape[1]):
        at = lax.broadcasted_iota(I32, (pos_ref.shape[0], rows.shape[0]), 1) + start
        pick = one_hot(at == pos_ref[:, k : k + 1])
        part = weights_ref[:, k : k + 1] * dot(pick, rows)
        total = part if total is None else total + part
    return total


def first_mix_kernel(pos_ref, weights_ref, *refs):
    refs[-1][...] = weigh(0, pos_ref, weights_ref, refs[:-1])


def last_mix_kernel(start, pos_ref, weights_ref, sofar_ref, *refs):
    refs[-1][...] = (sofar_ref[...] + weigh(start, pos_ref, weights_ref, refs[:-1])).astype(BF16)


def settle_kernel(in_ref, out_ref):
    out_ref[...] = jnp.maximum(in_ref[...], 0)


def call(kernel, out, operands, limit, specs=None):
    return pl.pallas_call(
        kernel,
        out_shape=out,
        in_specs=specs or [VMEM] * len(operands),
        out_specs=jax.tree.map(lambda _: VMEM, out),
        compiler_params=pltpu.CompilerParams(vmem_limit_bytes=limit * MIB),
    )(*operands)


def per_device(tokens, norm_gain, expert_ids, route_weights, w_gate, w_up, w_down):
    tok_rows, width = tokens.shape
    top_count = expert_ids.shape[1]
    ep_size, tp_size = lax.axis_size("ep"), lax.axis_size("tp")
    experts = w_gate.shape[0] * ep_size
    slots = 3 * tok_rows * top_count // (2 * experts)

    def sds(shape, dtype):
        return jax.ShapeDtypeStruct(shape, dtype)

    order = [0]
    for d in range(1, ep_size // 2 + 1):
        order += [d] if 2 * d == ep_size else [d, -d]
    first = 2 * 11 + 1
    hops = 2

    me = lax.axis_index("ep").astype(I32)[None]
    pos, block, own = call(
        lambda *refs: place_kernel(experts, slots, *refs),
        (
            sds((top_count, tok_rows), I32),
            sds((tok_rows + 8, width), BF16),
            sds((2 * slots, width), BF16),
        ),
        (me, expert_ids.T, tokens, norm_gain[None, :]),
        24,
        [SMEM, VMEM, VMEM, VMEM],
    )

    swap = [(i, (i + 1) % tp_size) for i in range(tp_size)]

    def whole(w, axis):
        other = lax.ppermute(w, "tp", swap)
        return jnp.concatenate([w, other], axis=axis)

    def shift(rows, d):
        if d == 0:
            return rows
        return lax.ppermute(rows, "ep", [(i, (i + d) % ep_size) for i in range(ep_size)])

    gate_full, up_full, down_full = whole(w_gate[0], 1), whole(w_up[0], 1), whole(w_down[0], 0)

    def expert(rows):
        hidden = (jax.nn.silu(dot(rows, gate_full)) * dot(rows, up_full)).astype(BF16)
        return dot(hidden, down_full).astype(BF16)

    parts = ((0, first), (first, len(order)))
    arrived, back, result = [None] * len(order), [None] * len(order), None
    arrived[0] = own[:slots]
    rows = {1: block, -1: block}
    for hop in range(1, hops + 1):
        rows = {sign: shift(rows[sign], sign) for sign in rows}
        if hop == 1:
            arrived[-1] = shift(own[slots:], ep_size // 2)
        reach = ep_size // 2 - hops if hop == hops else 1
        for sign in rows:
            picked = call(
                functools.partial(relay_kernel, experts, slots, sign),
                sds((reach * slots, width), BF16),
                (me, rows[sign]),
                24,
                [SMEM, VMEM],
            )
            arrived[order.index(sign * hop)] = picked[:slots]
            for s in range(1, reach):
                i = order.index(sign * (hop + s))
                arrived[i] = shift(picked[s * slots : (s + 1) * slots], sign * s)
    for lo, hi in parts:
        if result is not None:
            arrived, _ = lax.optimization_barrier((arrived, result))
        result = expert(jnp.concatenate(arrived[lo:hi], axis=0))
        for i in range(lo, hi):
            back[i] = shift(result[(i - lo) * slots : (i - lo + 1) * slots], -order[i])
    pos = call(settle_kernel, sds(pos.shape, I32), (pos,), 1)
    cols = pos.T
    sofar = call(
        first_mix_kernel,
        sds((tok_rows, width), F32),
        (cols, route_weights, *back[:first]),
        24,
    )
    return call(
        lambda *refs: last_mix_kernel(first * slots, *refs),
        sds((tok_rows, width), BF16),
        (cols, route_weights, sofar, *back[first:]),
        24,
    )


def solution(mesh):
    in_specs = (
        P(("grp", "ep", "tp"), None),
        P(),
        P(("grp", "ep", "tp"), None),
        P(("grp", "ep", "tp"), None),
        P("ep", None, "tp"),
        P("ep", None, "tp"),
        P("ep", "tp", None),
    )
    out_specs = P(("grp", "ep", "tp"), None)

    return jax.shard_map(
        per_device, mesh=mesh, in_specs=in_specs, out_specs=out_specs, check_vma=False
    )
```
